32 devices in a mesh: sp: 8 (over z, y), tp: 4 (over x, core).
Axes of the slice: x: 2, y: 2, z: 4, core: 2. Of those that a mesh axis runs over, the one named last changes fastest.
Arguments:
- inputs: bfloat16 [8192, 2048], P('sp'), may hold values from -6 to 6
- norm_gain: float32 [3, 2048], replicated, may hold values from 0.1 to 1.9
- query_weight: bfloat16 [3, 2048, 1024], P(None, 'sp', 'tp'), may hold values from -64 to 64
- key_weight: bfloat16 [3, 2048, 512], P(None, 'sp', 'tp'), may hold values from -4 to 4
- value_weight: bfloat16 [3, 2048, 512], P(None, 'sp', 'tp'), may hold values from -0.125 to 0.125
- output_weight: bfloat16 [3, 2048, 1024], P(None, 'sp', 'tp'), may hold values from -0.1875 to 0.1875
- sink_logit: float32 [3, 16], P(None, 'tp'), may hold values from 2 to 7
- final_gain: float32 [2048], replicated, may hold values from 0.1 to 1.9
Outputs:
- result: float32 [8192, 2048], P(('sp', 'tp'))
The draws below stay inside these ranges and needn't reach their ends.
All inputs are finite; a program needn't handle non-finite values.
Results may differ from the reference program's by a relative error of at most 0.015.
Values may be sent and summed in bfloat16 or wider, within the bound.
A program may use at most 64 MiB of HBM per device.

```python
import jax
import jax.numpy as jnp
from jax import lax

D = 2048
HEADS = 16
KV_HEADS = 8
HEAD_DIM = 64
WINDOW = 128
LAYERS = 3
TOK_DEV = 1024
SEQ = 8192


def shared_keys(key):
    base_key = jax.random.fold_in(key, 7)
    shape = (LAYERS, D, KV_HEADS * HEAD_DIM)
    return jnp.clip(jax.random.normal(base_key, shape, jnp.float32), -4.0, 4.0)


def draw_key_weight(key, part):
    return shared_keys(key).astype(jnp.bfloat16)


def draw_query_weight(key, part):
    base_key = jax.random.fold_in(key, 13)
    drawn = jax.random.normal(base_key, (LAYERS, D, HEADS * HEAD_DIM), jnp.float32)
    return jnp.clip(drawn, -4.0, 4.0).astype(jnp.bfloat16)


def level_of(key, dims, shards, smallest, high):
    loudness = 1.0
    for position, parts in shards:
        draws = jax.random.uniform(jax.random.fold_in(jax.random.fold_in(key, 6), position), (parts,), jnp.float32, smallest / len(shards), high / len(shards))
        loudness = loudness * jnp.repeat(jnp.exp(draws), dims[position] // parts).reshape((-1,) + (1,) * (len(dims) - 1 - position))
    return loudness


def bell_draw(own_key, extent, deviation, bound, cuts=(), kind=jnp.bfloat16):
    values = jax.random.normal(own_key, extent, jnp.float32) * deviation
    if len(cuts) > 0:
        values = level_of(own_key, extent, cuts, -0.22, 0.18) * values
    return jnp.clip(values, min=-bound, max=bound).astype(kind)


def setup_inputs(seed: int = 0) -> dict:
    streams_of = jax.random.split(jax.random.key(seed), 9)
    inputs = bell_draw(streams_of[0], (SEQ, D), 1.0, 6.0, ((0, 8),))
    norm_gain = jnp.clip(1.0 + 0.18 * jax.random.normal(streams_of[1], (LAYERS, D), jnp.float32), 0.1, 1.9)
    query_weight = draw_query_weight(jax.random.fold_in(streams_of[8], 71), 0)
    key_weight = draw_key_weight(jax.random.fold_in(streams_of[8], 71), 0)
    value_weight = bell_draw(streams_of[4], (LAYERS, D, KV_HEADS * HEAD_DIM), D ** -0.5, 0.125, ((1, 8), (2, 4)))
    output_weight = bell_draw(streams_of[5], (LAYERS, D, HEADS * HEAD_DIM), (HEADS * HEAD_DIM) ** -0.5, 0.1875, ((1, 8), (2, 4)))
    sink_logit = jnp.clip(2.0 + 5.0 * jax.random.uniform(streams_of[6], (LAYERS, HEADS), jnp.float32) ** level_of(streams_of[6], (LAYERS, HEADS), ((1, 4),), -0.2, 0.2), 2.0, 7.0)
    final_gain = jnp.clip(1.0 + 0.18 * jax.random.normal(streams_of[7], (D,), jnp.float32), 0.1, 1.9)
    return {"inputs": inputs, "norm_gain": norm_gain, "query_weight": query_weight, "key_weight": key_weight, "value_weight": value_weight, "output_weight": output_weight, "sink_logit": sink_logit, "final_gain": final_gain}


EPS = 1e-06

def norm_rows(values, gain):
    wide_values = values.astype(jnp.float32)
    inv_root = lax.rsqrt(lax.optimization_barrier(jnp.mean(wide_values * wide_values, axis=-1, keepdims=True)) + EPS)
    return wide_values * inv_root * gain

def rotate(values, places):
    half_dim = values.shape[-1] // 2
    inverse = 10000.0 ** (-jnp.arange(half_dim).astype(jnp.float32) / half_dim)
    angles = places[:, None] * inverse[None, :]
    cosine_table = jnp.cos(angles)[:, None, :]
    sine_table = jnp.sin(angles)[:, None, :]
    front_half = values[..., :half_dim]
    back_half = values[..., half_dim:]
    return jnp.concatenate([front_half * cosine_table - back_half * sine_table, back_half * cosine_table + front_half * sine_table], axis=-1)

def attend(queries, key_rows, value_rows, sink_row, allowed):
    scores = jnp.einsum('qkgd,skd->kgqs', queries.astype(jnp.float32), key_rows.astype(jnp.float32)) * queries.shape[-1] ** (-0.5)
    scores = jnp.where(allowed[None, None], scores, -jnp.inf)
    sink_col = sink_row[:, :, None]
    largest = jnp.maximum(lax.optimization_barrier(jnp.max(scores, axis=-1)), sink_col)
    powers = jnp.exp(scores - largest[..., None])
    denominator = lax.optimization_barrier(jnp.sum(powers, axis=-1)) + jnp.exp(sink_col - largest)
    weights = (powers / denominator[..., None]).astype(jnp.bfloat16)
    blended = jnp.einsum('kgqs,skd->qkgd', weights.astype(jnp.float32), value_rows.astype(jnp.float32))
    return blended.astype(jnp.bfloat16)

def reference(inputs, norm_gain, query_weight, key_weight, value_weight, output_weight, sink_logit, final_gain):
    seq_total = inputs.shape[0]
    blocks = seq_total // TOK_DEV
    per_group = HEADS // KV_HEADS
    places = jnp.arange(seq_total).astype(jnp.float32)
    current = inputs
    for layer in range(LAYERS):
        normed = norm_rows(current, norm_gain[layer]).astype(jnp.bfloat16)
        query_raw = jnp.dot(normed, query_weight[layer], preferred_element_type=jnp.float32) * float(D) ** (-0.5)
        key_raw = jnp.dot(normed, key_weight[layer], preferred_element_type=jnp.float32) * float(D) ** (-0.5)
        value_raw = jnp.dot(normed, value_weight[layer], preferred_element_type=jnp.float32)
        queries = rotate(query_raw.reshape(seq_total, HEADS, HEAD_DIM), places).astype(jnp.bfloat16)
        queries = queries.reshape(seq_total, KV_HEADS, per_group, HEAD_DIM)
        key_rot = rotate(key_raw.reshape(seq_total, KV_HEADS, HEAD_DIM), places).astype(jnp.bfloat16)
        value_all = value_raw.astype(jnp.bfloat16).reshape(seq_total, KV_HEADS, HEAD_DIM)
        padding = ((WINDOW, WINDOW), (0, 0), (0, 0))
        pad_keys = jnp.pad(key_rot, padding)
        pad_values = jnp.pad(value_all, padding)
        sink_row = sink_logit[layer].reshape(KV_HEADS, per_group)

        def one_block(block_index):
            first_row = block_index * TOK_DEV
            block_queries = lax.dynamic_slice_in_dim(queries, first_row, TOK_DEV, 0)
            block_keys = lax.dynamic_slice_in_dim(pad_keys, first_row, TOK_DEV + 2 * WINDOW, 0)
            block_values = lax.dynamic_slice_in_dim(pad_values, first_row, TOK_DEV + 2 * WINDOW, 0)
            query_pos = first_row + jnp.arange(TOK_DEV, dtype=jnp.int32)
            key_pos = first_row - WINDOW + jnp.arange(TOK_DEV + 2 * WINDOW, dtype=jnp.int32)
            allowed = (jnp.abs(key_pos[None, :] - query_pos[:, None]) <= WINDOW) & (key_pos[None, :] >= 0) & (key_pos[None, :] < seq_total)
            return attend(block_queries, block_keys, block_values, sink_row, allowed)
        attended = lax.map(one_block, jnp.arange(blocks, dtype=jnp.int32)).reshape(seq_total, HEADS * HEAD_DIM)
        current = jnp.dot(attended, output_weight[layer].T, preferred_element_type=jnp.float32).astype(jnp.bfloat16)
    return norm_rows(current, final_gain)
```

```python
import functools

import jax
import jax.numpy as jnp
from jax import lax
from jax.experimental import pallas as pl
from jax.experimental.pallas import tpu as pltpu
from jax.sharding import PartitionSpec as P

HEAD_DIM = 64
WINDOW = 128
EPS = 1e-06
AXES = ("sp", "tp")
F32 = jnp.float32
BF16 = jnp.bfloat16
VMEM_LIMIT = 48 * 1024 * 1024


def project_kernel(cur_ref, gain_ref, w_ref, cos_ref, sin_ref, q_ref, kv_ref, normed):
    @pl.when(pl.program_id(0) == 0)
    def _():
        wide = cur_ref[...].astype(F32)
        inv_root = lax.rsqrt(jnp.mean(wide * wide, axis=-1, keepdims=True) + EPS)
        normed[...] = (wide * inv_root * gain_ref[...]).astype(BF16)

    pieces, rows, width = w_ref.shape[0], w_ref.shape[3], w_ref.shape[4]
    acc = jnp.zeros((cur_ref.shape[0], width), F32)
    for s in range(pieces):
        acc += jnp.dot(
            normed[:, s * rows : (s + 1) * rows], w_ref[s, 0, 0], preferred_element_type=F32
        )
    half = HEAD_DIM // 2
    lane = lax.broadcasted_iota(jnp.int32, acc.shape, 1)
    front = (lane % HEAD_DIM) < half
    partner = jnp.where(front, pltpu.roll(acc, width - half, 1), pltpu.roll(acc, half, 1))
    turned = (acc * cos_ref[...] + partner * sin_ref[...]).astype(BF16)
    q_ref[0] = turned[:, : width // 2]
    kv_ref[0] = turned[:, width // 2 :]


def attend_kernel(layer, last, seq_total, sink_ref, off_ref, q_ref, kv_ref, lo_ref, hi_ref, w_ref, gain_ref, out_ref, acc):
    t = pl.program_id(0)
    tokens, cols = q_ref.shape[1], q_ref.shape[2]
    heads = cols // HEAD_DIM
    kv_cols = kv_ref.shape[2] // 2
    groups = kv_cols // HEAD_DIM
    per_group = heads // groups
    block = WINDOW
    span = block + 2 * WINDOW
    keys = jnp.concatenate([lo_ref[0], kv_ref[0], hi_ref[0]], axis=0)
    q_all = q_ref[0]
    i_pos = lax.broadcasted_iota(jnp.int32, (per_group * block, span), 0) % block
    j_pos = lax.broadcasted_iota(jnp.int32, (per_group * block, span), 1) - WINDOW
    near = jnp.abs(i_pos - j_pos) <= WINDOW
    row_head = lax.broadcasted_iota(jnp.int32, (per_group * block, 1), 0) // block
    parts = []
    for b in range(tokens // block):
        key_pos = off_ref[0] + b * block + j_pos
        allowed = near & (key_pos >= 0) & (key_pos < seq_total)
        heads_out = []
        for g in range(groups):
            lanes = slice(g * HEAD_DIM, (g + 1) * HEAD_DIM)
            here = slice(b * block, b * block + span)
            k = keys[here, lanes]
            v = keys[here, kv_cols + g * HEAD_DIM : kv_cols + (g + 1) * HEAD_DIM]
            q = jnp.concatenate(
                [
                    q_all[b * block : (b + 1) * block, h * HEAD_DIM : (h + 1) * HEAD_DIM]
                    for h in range(g * per_group, (g + 1) * per_group)
                ],
                axis=0,
            )
            scores = lax.dot_general(q, k, (((1,), (1,)), ((), ())), preferred_element_type=F32)
            scores = jnp.where(allowed, scores, -jnp.inf)
            sink = jnp.zeros((per_group * block, 1), F32)
            for e in range(per_group):
                sink = jnp.where(row_head == e, sink_ref[layer, t * heads + g * per_group + e], sink)
            largest = jnp.maximum(jnp.max(scores, axis=-1, keepdims=True), sink)
            powers = jnp.exp(scores - largest)
            total = jnp.sum(powers, axis=-1, keepdims=True) + jnp.exp(sink - largest)
            weights = (powers * (1.0 / total)).astype(BF16)
            mixed = jnp.dot(weights, v, preferred_element_type=F32).astype(BF16)
            heads_out += [mixed[e * block : (e + 1) * block] for e in range(per_group)]
        parts.append(jnp.concatenate(heads_out, axis=1))
    attended = jnp.concatenate(parts, axis=0)
    rows = w_ref.shape[3]
    for s in range(w_ref.shape[0]):
        piece = lax.dot_general(
            attended, w_ref[s, 0, 0], (((1,), (1,)), ((), ())), preferred_element_type=F32
        )
        where = slice(s * rows, (s + 1) * rows)

        @pl.when(t == 0)
        def _():
            acc[:, where] = piece

        @pl.when(t > 0)
        def _():
            acc[:, where] += piece

    @pl.when(t == pl.num_programs(0) - 1)
    def _():
        state = acc[...].astype(BF16)
        if last:
            wide = state.astype(F32)
            inv_root = lax.rsqrt(jnp.mean(wide * wide, axis=-1, keepdims=True) + EPS)
            out_ref[...] = wide * inv_root * gain_ref[...]
        else:
            out_ref[...] = state


def gather_weights(packed):
    count = lax.axis_size("sp") * lax.axis_size("tp")
    whole = lax.all_gather(packed, AXES, axis=0, tiled=False)
    return whole.reshape((lax.axis_size("sp"), lax.axis_size("tp")) + packed.shape)


def shards(
    inputs, norm_gain, query_weight, key_weight, value_weight, output_weight, sink_logit, final_gain
):
    n_sp, n_tp = lax.axis_size("sp"), lax.axis_size("tp")
    layers, rows, cols = query_weight.shape
    features = inputs.shape[1]
    tokens = inputs.shape[0] // n_tp
    width = 2 * cols
    place = lax.axis_index("sp") * n_tp + lax.axis_index("tp")
    offset = place * tokens
    seq_total = tokens * n_sp * n_tp
    whole = gather_weights(
        jnp.concatenate([query_weight, key_weight, value_weight, output_weight], axis=2)
    )
    sinks = lax.all_gather(sink_logit, "tp", axis=1, tiled=True)

    half = HEAD_DIM // 2
    inverse = 10000.0 ** (-jnp.arange(half).astype(F32) / half)
    places = (offset + jnp.arange(tokens, dtype=jnp.int32)).astype(F32)
    angles = places[:, None] * inverse[None, :]
    cosine, sine = jnp.cos(angles), jnp.sin(angles)
    scale = float(features) ** (-0.5)
    root = HEAD_DIM ** (-0.5)
    pair_c = jnp.concatenate([cosine, cosine], axis=1) * scale
    pair_s = jnp.concatenate([-sine, sine], axis=1) * scale
    kv_cols = key_weight.shape[2]
    heads, groups = cols // HEAD_DIM, kv_cols // HEAD_DIM
    one = jnp.ones((tokens, kv_cols), F32)
    cos_table = jnp.concatenate([jnp.tile(pair_c * root, (1, heads)), jnp.tile(pair_c, (1, groups)), one], axis=1)
    sin_table = jnp.concatenate([jnp.tile(pair_s * root, (1, heads)), jnp.tile(pair_s, (1, groups)), 0 * one], axis=1)
    offset_row = jnp.reshape(offset, (1,)).astype(jnp.int32)

    count = n_sp * n_tp
    forward = [(i, i + 1) for i in range(count - 1)]
    backward = [(b, a) for a, b in forward]
    current = lax.dynamic_slice_in_dim(inputs, lax.axis_index("tp") * tokens, tokens, 0)
    full = lambda *shape: pl.BlockSpec(shape, lambda t: (0,) * len(shape))
    smem = pl.BlockSpec(memory_space=pltpu.SMEM)
    for layer in range(layers):
        last = layer == layers - 1
        queries, kv = pl.pallas_call(
            project_kernel,
            name="project",
            grid=(n_tp,),
            out_shape=[jax.ShapeDtypeStruct((n_tp, tokens, cols), BF16)] * 2,
            in_specs=[
                full(tokens, features),
                full(1, features),
                pl.BlockSpec((n_sp, 1, 1, rows, width), lambda t, l=layer: (0, t, l, 0, 0)),
                full(tokens, width),
                full(tokens, width),
            ],
            out_specs=[pl.BlockSpec((1, tokens, cols), lambda t: (t, 0, 0))] * 2,
            scratch_shapes=[pltpu.VMEM((tokens, features), BF16)],
            compiler_params=pltpu.CompilerParams(vmem_limit_bytes=VMEM_LIMIT),
        )(current, norm_gain[layer : layer + 1], whole, cos_table, sin_table)
        low = lax.ppermute(kv[:, tokens - WINDOW :], AXES, forward)
        high = lax.ppermute(kv[:, :WINDOW], AXES, backward)
        current = pl.pallas_call(
            functools.partial(attend_kernel, layer, last, seq_total),
            name="attend",
            grid=(n_tp,),
            out_shape=jax.ShapeDtypeStruct((tokens, features), F32 if last else BF16),
            in_specs=[
                smem,
                smem,
                pl.BlockSpec((1, tokens, cols), lambda t: (t, 0, 0)),
                pl.BlockSpec((1, tokens, cols), lambda t: (t, 0, 0)),
                pl.BlockSpec((1, WINDOW, cols), lambda t: (t, 0, 0)),
                pl.BlockSpec((1, WINDOW, cols), lambda t: (t, 0, 0)),
                pl.BlockSpec((n_sp, 1, 1, rows, cols), lambda t, l=layer: (0, t, l, 0, 2)),
                full(1, features),
            ],
            out_specs=full(tokens, features),
            scratch_shapes=[pltpu.VMEM((tokens, features), F32)],
            compiler_params=pltpu.CompilerParams(vmem_limit_bytes=VMEM_LIMIT),
        )(sinks, offset_row, queries, kv, low, high, whole, final_gain[None])
    return current


def solution(mesh):
    in_specs = (
        P("sp", None),
        P(),
        P(None, "sp", "tp"),
        P(None, "sp", "tp"),
        P(None, "sp", "tp"),
        P(None, "sp", "tp"),
        P(None, "tp"),
        P(),
    )
    out_specs = P(("sp", "tp"), None)
    return jax.shard_map(shards, mesh=mesh, in_specs=in_specs, out_specs=out_specs, check_vma=False)
```

```python
import functools

import jax
import jax.numpy as jnp
from jax import lax
from jax.experimental import pallas as pl
from jax.experimental.pallas import tpu as pltpu
from jax.sharding import PartitionSpec as P

HEAD_DIM = 64
WINDOW = 128
EPS = 1e-06
AXES = ("sp", "tp")
F32 = jnp.float32
BF16 = jnp.bfloat16
VMEM_LIMIT = 48 * 1024 * 1024


def project_kernel(cur_ref, gain_ref, w_ref, cos_ref, sin_ref, q_ref, kv_ref, normed):
    @pl.when(pl.program_id(0) == 0)
    def _():
        wide = cur_ref[...].astype(F32)
        inv_root = lax.rsqrt(jnp.mean(wide * wide, axis=-1, keepdims=True) + EPS)
        normed[...] = (wide * inv_root * gain_ref[...]).astype(BF16)

    pieces, rows, width = w_ref.shape[0], w_ref.shape[3], w_ref.shape[4]
    acc = jnp.zeros((cur_ref.shape[0], width), F32)
    for s in range(pieces):
        acc += jnp.dot(
            normed[:, s * rows : (s + 1) * rows], w_ref[s, 0, 0], preferred_element_type=F32
        )
    half = HEAD_DIM // 2
    lane = lax.broadcasted_iota(jnp.int32, acc.shape, 1)
    front = (lane % HEAD_DIM) < half
    partner = jnp.where(front, pltpu.roll(acc, width - half, 1), pltpu.roll(acc, half, 1))
    turned = (acc * cos_ref[...] + partner * sin_ref[...]).astype(BF16)
    q_ref[0] = turned[:, : width // 2]
    kv_ref[0] = turned[:, width // 2 :]


def attend_kernel(layer, last, sink_ref, q_ref, kv_ref, lo_ref, hi_ref, bias_ref, whole_ref, gain_ref, out_ref, w_ref, attended, acc, w_sem):
    t = pl.program_id(0)
    tokens, cols = q_ref.shape[1], q_ref.shape[2]
    load = pltpu.make_async_copy(
        whole_ref.at[:, :, layer, :, pl.ds(2 * cols, cols)], w_ref, w_sem
    )

    @pl.when(t == 0)
    def _():
        load.start()

    heads = cols // HEAD_DIM
    kv_cols = kv_ref.shape[2] // 2
    groups = kv_cols // HEAD_DIM
    per_group = heads // groups
    block = WINDOW
    span = block + 2 * WINDOW
    keys = jnp.concatenate([lo_ref[0], kv_ref[0], hi_ref[0]], axis=0)
    q_all = q_ref[0]
    row_head = lax.broadcasted_iota(jnp.int32, (per_group * block, 1), 0) // block
    for b in range(tokens // block):
        here = slice(b * block, (b + 1) * block)
        bias = jnp.concatenate([bias_ref[here]] * per_group, axis=0)
        near = slice(b * block, b * block + span)
        for g in range(groups):
            k = keys[near, g * HEAD_DIM : (g + 1) * HEAD_DIM]
            v = keys[near, kv_cols + g * HEAD_DIM : kv_cols + (g + 1) * HEAD_DIM]
            first = g * per_group
            q = jnp.concatenate(
                [
                    q_all[here, h * HEAD_DIM : (h + 1) * HEAD_DIM]
                    for h in range(first, first + per_group)
                ],
                axis=0,
            )
            scores = lax.dot_general(q, k, (((1,), (1,)), ((), ())), preferred_element_type=F32)
            scores = scores + bias
            sink = jnp.zeros((per_group * block, 1), F32)
            for e in range(per_group):
                sink = jnp.where(row_head == e, sink_ref[layer, t * heads + first + e], sink)
            largest = jnp.maximum(jnp.max(scores, axis=-1, keepdims=True), sink)
            powers = jnp.exp(scores - largest)
            total = jnp.sum(powers, axis=-1, keepdims=True) + jnp.exp(sink - largest)
            mixed = jnp.dot(powers.astype(BF16), v, preferred_element_type=F32) * (1.0 / total)
            mixed = mixed.astype(BF16)
            attended[t, here, first * HEAD_DIM : (first + per_group) * HEAD_DIM] = jnp.concatenate(
                [mixed[e * block : (e + 1) * block] for e in range(per_group)], axis=1
            )

    @pl.when(t == pl.num_programs(0) - 1)
    def _():
        load.wait()
        rows = w_ref.shape[2]
        for s in range(w_ref.shape[0]):
            piece = jnp.zeros((tokens, rows), F32)
            for u in range(w_ref.shape[1]):
                piece += lax.dot_general(
                    attended[u], w_ref[s, u], (((1,), (1,)), ((), ())), preferred_element_type=F32
                )
            where = slice(s * rows, (s + 1) * rows)
            if last:
                acc[:, where] = piece.astype(BF16)
            else:
                out_ref[:, where] = piece.astype(BF16)
        if last:
            wide = acc[...].astype(F32)
            inv_root = lax.rsqrt(jnp.mean(wide * wide, axis=-1, keepdims=True) + EPS)
            out_ref[...] = wide * inv_root * gain_ref[...]


def gather_weights(packed):
    count = lax.axis_size("sp") * lax.axis_size("tp")
    whole = lax.all_gather(packed, AXES, axis=0, tiled=False)
    return whole.reshape((lax.axis_size("sp"), lax.axis_size("tp")) + packed.shape)


def shards(
    inputs, norm_gain, query_weight, key_weight, value_weight, output_weight, sink_logit, final_gain
):
    n_sp, n_tp = lax.axis_size("sp"), lax.axis_size("tp")
    layers, rows, cols = query_weight.shape
    features = inputs.shape[1]
    tokens = inputs.shape[0] // n_tp
    width = 2 * cols
    place = lax.axis_index("sp") * n_tp + lax.axis_index("tp")
    offset = place * tokens
    seq_total = tokens * n_sp * n_tp
    whole = gather_weights(
        jnp.concatenate([query_weight, key_weight, value_weight, output_weight], axis=2)
    )
    sinks = lax.all_gather(sink_logit, "tp", axis=1, tiled=True)
    whole, sinks = lax.optimization_barrier((whole, sinks))

    half = HEAD_DIM // 2
    inverse = 10000.0 ** (-jnp.arange(half).astype(F32) / half)
    places = (offset + jnp.arange(tokens, dtype=jnp.int32)).astype(F32)
    angles = places[:, None] * inverse[None, :]
    cosine, sine = jnp.cos(angles), jnp.sin(angles)
    scale = float(features) ** (-0.5)
    root = HEAD_DIM ** (-0.5)
    pair_c = jnp.concatenate([cosine, cosine], axis=1) * scale
    pair_s = jnp.concatenate([-sine, sine], axis=1) * scale
    kv_cols = key_weight.shape[2]
    heads, groups = cols // HEAD_DIM, kv_cols // HEAD_DIM
    one = jnp.ones((tokens, kv_cols), F32)
    cos_table = jnp.concatenate([jnp.tile(pair_c * root, (1, heads)), jnp.tile(pair_c, (1, groups)), one], axis=1)
    sin_table = jnp.concatenate([jnp.tile(pair_s * root, (1, heads)), jnp.tile(pair_s, (1, groups)), 0 * one], axis=1)
    span = 3 * WINDOW
    row = jnp.arange(tokens, dtype=jnp.int32)[:, None]
    reach = jnp.arange(span, dtype=jnp.int32)[None, :] - WINDOW
    key_pos = offset + row - row % WINDOW + reach
    allowed = (jnp.abs(row % WINDOW - reach) <= WINDOW) & (key_pos >= 0) & (key_pos < seq_total)
    bias = jnp.where(allowed, 0.0, -jnp.inf).astype(F32)

    count = n_sp * n_tp
    forward = [(i, i + 1) for i in range(count - 1)]
    backward = [(b, a) for a, b in forward]
    current = lax.dynamic_slice_in_dim(inputs, lax.axis_index("tp") * tokens, tokens, 0)
    full = lambda *shape: pl.BlockSpec(shape, lambda t: (0,) * len(shape))
    smem = pl.BlockSpec(memory_space=pltpu.SMEM)
    for layer in range(layers):
        last = layer == layers - 1
        queries, kv = pl.pallas_call(
            project_kernel,
            name="project",
            grid=(n_tp,),
            out_shape=[jax.ShapeDtypeStruct((n_tp, tokens, cols), BF16)] * 2,
            in_specs=[
                full(tokens, features),
                full(1, features),
                pl.BlockSpec((n_sp, 1, 1, rows, width), lambda t, l=layer: (0, t, l, 0, 0)),
                full(tokens, width),
                full(tokens, width),
            ],
            out_specs=[pl.BlockSpec((1, tokens, cols), lambda t: (t, 0, 0))] * 2,
            scratch_shapes=[pltpu.VMEM((tokens, features), BF16)],
            compiler_params=pltpu.CompilerParams(vmem_limit_bytes=VMEM_LIMIT),
        )(current, norm_gain[layer : layer + 1], whole, cos_table, sin_table)
        low = lax.ppermute(kv[:, tokens - WINDOW :], AXES, forward)
        high = lax.ppermute(kv[:, :WINDOW], AXES, backward)
        current = pl.pallas_call(
            functools.partial(attend_kernel, layer, last),
            name="attend",
            grid=(n_tp,),
            out_shape=jax.ShapeDtypeStruct((tokens, features), F32 if last else BF16),
            in_specs=[
                smem,
                pl.BlockSpec((1, tokens, cols), lambda t: (t, 0, 0)),
                pl.BlockSpec((1, tokens, cols), lambda t: (t, 0, 0)),
                pl.BlockSpec((1, WINDOW, cols), lambda t: (t, 0, 0)),
                pl.BlockSpec((1, WINDOW, cols), lambda t: (t, 0, 0)),
                full(tokens, span),
                pl.BlockSpec(memory_space=pl.ANY),
                full(1, features),
            ],
            out_specs=full(tokens, features),
            scratch_shapes=[
                pltpu.VMEM((n_sp, n_tp, rows, cols), BF16),
                pltpu.VMEM((n_tp, tokens, cols), BF16),
                pltpu.VMEM((tokens, features), BF16),
                pltpu.SemaphoreType.DMA,
            ],
            compiler_params=pltpu.CompilerParams(vmem_limit_bytes=VMEM_LIMIT),
        )(sinks, queries, kv, low, high, bias, whole, final_gain[None])
    return current


def solution(mesh):
    in_specs = (
        P("sp", None),
        P(),
        P(None, "sp", "tp"),
        P(None, "sp", "tp"),
        P(None, "sp", "tp"),
        P(None, "sp", "tp"),
        P(None, "tp"),
        P(),
    )
    out_specs = P(("sp", "tp"), None)
    return jax.shard_map(shards, mesh=mesh, in_specs=in_specs, out_specs=out_specs, check_vma=False)
```
